512 devices in a mesh: sp: 64 (over z, y), tp: 8 (over x, core).
Axes of the slice: x: 4, y: 8, z: 8, core: 2. Of those that a mesh axis runs over, the one named last changes fastest.
Arguments:
- resid: bfloat16 [32768, 2048], P(('sp', 'tp')), may hold values from -3 to 3
- queries: bfloat16 [32768, 1024], P('sp', 'tp'), may hold values from -6 to 6
- keys: bfloat16 [32768, 512], P('sp', 'tp'), may hold values from -6 to 6
- values: bfloat16 [32768, 512], P('sp', 'tp'), may hold values from -6 to 6
- documents: int32 [32768], P('sp'), may hold values from 0 to 31, never falling along the last dimension, each value on 1 to 2048 neighbouring positions
- sinks: float32 [16], P('tp'), may hold values from 0 to 5
- out_proj: bfloat16 [1024, 2048], replicated, may hold values from -0.75 to 0.75
- norm_gain: float32 [2048], replicated, may hold values from 0.1 to 1.9
- gate_proj: bfloat16 [2048, 5632], P('sp', 'tp'), may hold values from -0.125 to 0.125
- up_proj: bfloat16 [2048, 5632], P('sp', 'tp'), may hold values from -0.125 to 0.125
- down_proj: bfloat16 [5632, 2048], P('tp', 'sp'), may hold values from -0.078125 to 0.078125
Outputs:
- mixed: bfloat16 [32768, 2048], P(('sp', 'tp'))
The draws below stay inside these ranges and needn't reach their ends.
Inputs may be any that keep to these rules, and one draw needn't show every extreme that they name: `documents`: document numbers never fall along the sequence; each document holds at most 2048 positions.
All inputs are finite; a program needn't handle non-finite values.
Results may differ from the reference program's by a relative error of at most 0.0095.
Values may be sent and summed in bfloat16 or wider, within the bound.
A program may use at most 64 MiB of HBM per device.

```python
import math
import jax
import jax.numpy as jnp
import numpy as np
from jax import lax

D = 2048
FF = 5632
HEADS = 16
KV_HEADS = 8
HD = 64
WINDOW = 128
TOK_DEV = 512
TOKENS = 32768
DOCS = 32
N_TP = 8


def draw_pair(key):
    base = jax.random.fold_in(key, 17)
    first, second = jax.random.split(base, 2)
    queries = jnp.clip(jax.random.normal(first, (TOKENS, HEADS * HD), jnp.float32), -6.0, 6.0)
    keys = jnp.clip(jax.random.normal(second, (TOKENS, KV_HEADS * HD), jnp.float32), -6.0, 6.0)
    return (queries, keys)


def draw_queries(key, part):
    return draw_pair(key)[0].astype(jnp.bfloat16)


def draw_keys(key, part):
    return draw_pair(key)[1].astype(jnp.bfloat16)


def block_scale(stream_key, dims, cuts, low, top_value):
    loudness, own = 1.0, jax.random.fold_in(stream_key, 6)
    for position, shards_of in cuts:
        steps = jnp.exp(jax.random.uniform(jax.random.fold_in(own, position), (shards_of,), jnp.float32, low / len(cuts), top_value / len(cuts)))
        loudness = loudness * jnp.repeat(steps, dims[position] // shards_of).reshape([-1 if axis == position else 1 for axis in range(len(dims))])
    return loudness


def length_profile(amount, total, limit, skew):
    weights = [(1 << 20) // math.isqrt(rank ** skew) + 1 for rank in range(2, amount + 1)]
    surplus, given = total - limit - (amount - 1), [1] * (amount - 1)
    while surplus > 0:
        candidates = [i for i in range(amount - 1) if given[i] < limit]
        pool, remaining = sum([weights[i] for i in candidates]), surplus
        for i in candidates:
            addition = min(limit - given[i], max(1, remaining * weights[i] // pool), surplus)
            given[i] = given[i] + addition
            surplus = surplus - addition
    return np.array([limit] + given)


def uneven_parts(key, count, total, most, skew):
    if count == 2:
        one = jax.random.randint(key, (), max(1, total - most), min(most, total - 1) + 1)
        return jnp.stack([one, total - one])
    tallies = jnp.asarray(length_profile(count, total, most, skew), jnp.int32)
    twos = (count - 1) // 2
    giver, receiver = tallies[1:1 + 2 * twos:2], tallies[2:2 + 2 * twos:2]
    slack = jnp.minimum(giver - 1, most - receiver)
    shifted = jax.random.randint(jax.random.fold_in(key, 1), (twos,), 0, 1 << 20) % (slack + 1)
    tallies = tallies.at[1:1 + 2 * twos:2].set(giver - shifted).at[2:2 + 2 * twos:2].set(receiver + shifted)
    return tallies[jax.random.permutation(jax.random.fold_in(key, 2), count)]


def noise(key, shape, deviation, limit, cuts=(), held_as=jnp.bfloat16):
    loudness = block_scale(key, shape, cuts, -0.22, 0.18) if cuts else 1.0
    entries = jax.random.normal(key, shape, jnp.float32) * deviation * loudness
    return jnp.minimum(jnp.maximum(entries, -limit), limit).astype(held_as)


def setup_inputs(seed: int = 0) -> dict:
    splits = jax.random.split(jax.random.key(seed), 12)
    resid = noise(splits[0], (TOKENS, D), 0.5, 3.0, ((0, 512),))
    queries = draw_queries(jax.random.fold_in(splits[11], 71), 0)
    keys = draw_keys(jax.random.fold_in(splits[11], 71), 0)
    values = noise(splits[3], (TOKENS, KV_HEADS * HD), 1.0, 6.0, ((0, 64), (1, 8)))
    documents = jnp.searchsorted(jnp.cumsum(uneven_parts(splits[4], DOCS, TOKENS, 4 * TOK_DEV, 0)), jnp.arange(TOKENS), side="right").astype(jnp.int32)
    sinks = jnp.clip(5.0 * jax.random.uniform(splits[5], (HEADS,), jnp.float32) ** block_scale(splits[5], (HEADS,), ((0, 8),), -0.2, 0.2), 0.0, 5.0)
    out_proj = noise(splits[6], (HEADS * HD, D), HD ** -0.5, 0.75)
    norm_gain = jnp.clip(1.0 + 0.18 * jax.random.normal(splits[7], (D,), jnp.float32), 0.1, 1.9)
    gate_proj = noise(splits[8], (D, FF), D ** -0.5, 0.125, ((0, 64), (1, 8)))
    up_proj = noise(splits[9], (D, FF), D ** -0.5, 0.125, ((0, 64), (1, 8)))
    down_proj = noise(splits[10], (FF, D), FF ** -0.5, 0.078125, ((0, 8), (1, 64)))
    return {"resid": resid, "queries": queries, "keys": keys, "values": values, "documents": documents, "sinks": sinks, "out_proj": out_proj, "norm_gain": norm_gain, "gate_proj": gate_proj, "up_proj": up_proj, "down_proj": down_proj}


def band_attend(queries, keys, values, documents, sinks):
    rows = queries.shape[0]
    kv_heads = keys.shape[1] // HD
    group = queries.shape[1] // HD // kv_heads
    blocks = rows // WINDOW
    zero_keys = jnp.zeros((WINDOW, keys.shape[1]), jnp.float32)
    ext_keys = jnp.concatenate([zero_keys, keys.astype(jnp.float32)], axis=0).reshape(blocks + 1, WINDOW, kv_heads, HD)
    ext_values = jnp.concatenate([zero_keys, values.astype(jnp.float32)], axis=0).reshape(blocks + 1, WINDOW, kv_heads, HD)
    ext_docs = jnp.concatenate([jnp.zeros((WINDOW,), jnp.int32), documents.astype(jnp.int32)], axis=0).reshape(blocks + 1, WINDOW)
    band_keys = jnp.concatenate([ext_keys[:-1], ext_keys[1:]], axis=1)
    band_values = jnp.concatenate([ext_values[:-1], ext_values[1:]], axis=1)
    band_docs = jnp.concatenate([ext_docs[:-1], ext_docs[1:]], axis=1)
    query_docs = documents.reshape(blocks, WINDOW)
    distance = jnp.arange(WINDOW)[:, None] + WINDOW - jnp.arange(2 * WINDOW)[None, :]
    key_pos = jnp.arange(blocks)[:, None] * WINDOW + jnp.arange(2 * WINDOW)[None, :] - WINDOW
    visible = ((distance >= 0) & (distance < WINDOW))[None] & (key_pos >= 0)[:, None, :] & (band_docs[:, None, :] == query_docs[:, :, None])
    query_blocks = queries.astype(jnp.float32).reshape(blocks, WINDOW, kv_heads, group, HD)
    scores = jnp.einsum('nikgd,njkd->nkgij', query_blocks, band_keys) * HD ** (-0.5)
    scores = jnp.where(visible[:, None, None], scores, -jnp.inf)
    sink_logit = sinks.astype(jnp.float32).reshape(kv_heads, group)[None, :, :, None, None]
    row_top = jnp.maximum(lax.optimization_barrier(jnp.max(scores, axis=-1, keepdims=True)), sink_logit)
    raw_weights = jnp.exp(scores - row_top)
    totals = lax.optimization_barrier(jnp.sum(raw_weights, axis=-1, keepdims=True)) + jnp.exp(sink_logit - row_top)
    weights = (raw_weights / totals).astype(jnp.bfloat16).astype(jnp.float32)
    attended = jnp.einsum('nkgij,njkd->nikgd', weights, band_values)
    return attended.astype(jnp.bfloat16).reshape(rows, kv_heads * group * HD)

def reference(resid, queries, keys, values, documents, sinks, out_proj, norm_gain, gate_proj, up_proj, down_proj):
    group = HEADS // KV_HEADS
    pieces = []
    for head in range(KV_HEADS):
        pieces.append(band_attend(queries[:, head * group * HD:(head + 1) * group * HD], keys[:, head * HD:(head + 1) * HD], values[:, head * HD:(head + 1) * HD], documents, sinks[head * group:(head + 1) * group]))
    attended = jnp.concatenate(pieces, axis=1)
    mid_rows = resid.astype(jnp.float32) + jnp.dot(attended, out_proj, preferred_element_type=jnp.float32)
    scale = lax.rsqrt(lax.optimization_barrier(jnp.mean(mid_rows * mid_rows, axis=-1, keepdims=True)) + 1e-06)
    normed = (mid_rows * scale * norm_gain).astype(jnp.bfloat16)
    width = FF // N_TP

    def ffn_rows(row_block):
        gate_acts = jnp.dot(row_block, gate_proj, preferred_element_type=jnp.float32)
        up_acts = jnp.dot(row_block, up_proj, preferred_element_type=jnp.float32)
        hidden = (jax.nn.silu(gate_acts) * up_acts).astype(jnp.bfloat16)
        totals = jnp.zeros((row_block.shape[0], D), jnp.float32)
        for block in range(N_TP):
            partial_value = jnp.dot(hidden[:, block * width:(block + 1) * width], down_proj[block * width:(block + 1) * width], preferred_element_type=jnp.float32).astype(jnp.bfloat16)
            totals = totals + lax.optimization_barrier(partial_value).astype(jnp.float32)
        return totals
    summed = lax.map(ffn_rows, normed.reshape(TOKENS // TOK_DEV, TOK_DEV, D)).reshape(TOKENS, D)
    return (mid_rows + summed).astype(jnp.bfloat16)
```

```python
import jax
import jax.numpy as jnp
from jax import lax
from jax.experimental import pallas as pl
from jax.experimental.pallas import tpu as pltpu
from jax.sharding import PartitionSpec as P

MESH = pl.DeviceIdType.MESH
F32, BF16 = jnp.float32, jnp.bfloat16
SIDE = 8
REL = (0, -1, 1, -2, 2, -3, 3, -4)
LAST = {1: 4, -1: 3}
BOTH = (1, -1)
SEMS = 160


def wrap(value, offset):
    return lax.rem(value + (offset + SIDE), SIDE) if offset else value


def unit_of(stage, half, sign):
    if stage == 0:
        return half
    if stage == 4:
        return 14 + half
    return 4 * stage - 2 + 2 * half + (0 if sign > 0 else 1)


def dot(a, b):
    return jnp.dot(a, b, preferred_element_type=F32)


def dot_t(a, b):
    return lax.dot_general(a, b, (((1,), (1,)), ((), ())), preferred_element_type=F32)


def layer(
    sinks, resid, q, kt, vt, docs, gain, gu, dn, op_hbm, out,
    wg, wd, op, nb, at, ka, kb, va, vb, hk, hv, dh, ed, att, mid, hid,
    pb, pr, qb, rx, ss, tn, tt, send, recv, local,
):
    sp, tp = lax.axis_index("sp"), lax.axis_index("tp")
    y, z = lax.rem(sp, SIDE), lax.div(sp, SIDE)
    x, core = lax.rem(lax.div(tp, 2), 4), lax.rem(tp, 2)
    other = 1 - core
    partner = (sp, 2 * x + other)
    ahead = lax.rem(sp + 1, SIDE * SIDE)
    behind = lax.rem(sp + SIDE * SIDE - 1, SIDE * SIDE)

    def place(dy, dz):
        return (wrap(z, dz) * SIDE + wrap(y, dy), tp)

    def toward(half, ring, sign):
        return place(sign, 0) if half == ring else place(0, sign)

    def chip(j):
        return lax.rem(x + j, 4)

    barrier = pltpu.get_barrier_semaphore()
    greeted = [place(1, 0), place(-1, 0), place(0, 1), place(0, -1)]
    greeted += [(ahead, tp), (behind, tp)]
    greeted += [(sp, lax.rem(tp + j, 8)) for j in range(1, 8)]
    for where in greeted:
        pl.semaphore_signal(barrier, inc=1, device_id=where, device_id_type=MESH)

    own_op = pltpu.make_async_copy(op_hbm, op, local.at[0])
    own_gu = pltpu.make_async_copy(gu, wg.at[z, y], local.at[1])
    own_dn = [
        pltpu.make_async_copy(dn.at[pl.ds(16 * h, 16)], wd.at[h, 0], local.at[2 + h]) for h in (0, 1)
    ]
    for copy in (own_gu, *own_dn, own_op):
        copy.start()

    pl.semaphore_wait(barrier, len(greeted))

    pending = []

    def go(src, dst, where):
        n = len(pending)
        copy = pltpu.make_async_remote_copy(
            src_ref=src, dst_ref=dst, send_sem=send.at[n], recv_sem=recv.at[n],
            device_id=where, device_id_type=MESH,
        )
        copy.start()
        pending.append(copy)
        return copy

    def gu_at(half, near):
        rows = pl.ds(16 * half, 16)
        return wg.at[z, wrap(y, near), rows] if half == 0 else wg.at[wrap(z, near), y, rows]

    def gu_own(half):
        return gu.at[pl.ds(16 * half, 16)]

    def gu_part(half, far, part):
        rows, some = pl.ds(16 * half, 16), pl.ds(4 * part, 4)
        return wg.at[wrap(z, far), some, rows] if half == 0 else wg.at[some, wrap(y, far), rows]

    near_gu, far_gu, near_dn, far_dn = {}, {}, {}, {}

    def inject(half, near, src=None):
        block = gu_at(half, near)
        for sign in BOTH:
            far_gu[half, sign, near] = go(block if src is None else src, block, toward(half, 1, sign))

    def gu_step(k):
        for half in (0, 1):
            for sign in BOTH:
                if k > LAST[sign]:
                    continue
                near_gu[half, sign, k].wait_recv()
                block = gu_at(half, -sign * k)
                if k < LAST[sign]:
                    near_gu[half, sign, k + 1] = go(block, block, toward(half, 0, sign))
                inject(half, -sign * k)

    def gu_send(stage, half, sign, part):
        block = gu_part(half, -sign * (stage - 1), part)
        far_gu[stage, half, sign, part] = go(block, block, toward(half, 1, sign))

    def dn_first(half, sign, k, src=None):
        src = wd.at[half, REL.index(-sign * (k - 1))] if src is None else src
        near_dn[half, sign, k] = go(src, wd.at[half, REL.index(-sign * k)], toward(half, 0, sign))

    def dn_step(k):
        for half in (0, 1):
            for sign in BOTH:
                if k <= LAST[sign]:
                    near_dn[half, sign, k].wait_recv()
                    if k < LAST[sign]:
                        dn_first(half, sign, k + 1)

    def dn_send(stage, half, sign, part):
        some = pl.ds(4 * part, 4)
        far_dn[stage, half, sign, part] = go(
            wd.at[unit_of(stage - 1, half, sign), some],
            wd.at[unit_of(stage, half, sign), some],
            toward(half, 1, sign),
        )

    def dn_pass(stage, part):
        for half in (0, 1):
            for sign in BOTH:
                far_dn[stage, half, sign, part].wait_recv()
                if stage < 3 or part == (0 if sign > 0 else 1):
                    dn_send(stage + 1, half, sign, part)

    for half in (0, 1):
        for sign in BOTH:
            near_gu[half, sign, 1] = go(gu_own(half), gu_at(half, 0), toward(half, 0, sign))
    for half in (0, 1):
        inject(half, 0, gu_own(half))
    tail = pl.ds(384, 128)
    halo = [
        go(kt.at[:, tail], hk, (ahead, tp)),
        go(vt.at[:, tail], hv, (ahead, tp)),
        go(docs, dh, (ahead, tp)),
    ]

    for first, second, source in ((ka, kb, kt), (va, vb, vt)):
        first[64:128, :] = jnp.zeros((64, 640), BF16)
        second[0:64, :] = jnp.zeros((64, 640), BF16)
        first[0:64, 128:640] = source[...]
        second[64:128, 128:640] = source[...]
    for block in range(4):
        ed[0:1, 128 * (block + 1) : 128 * (block + 2)] = docs[block : block + 1, :].astype(F32)

    def attend(block):
        rows, span = pl.ds(128 * block, 128), pl.ds(128 * block, 256)
        query_docs = jnp.broadcast_to(ed[0:1, 128 * (block + 1) : 128 * (block + 2)], (128, 128)).T
        query_docs = jnp.concatenate([query_docs, query_docs], axis=1)
        at_query = lax.broadcasted_iota(jnp.int32, (128, 256), 0)
        at_key = lax.broadcasted_iota(jnp.int32, (128, 256), 1)
        visible = (at_key > at_query) & (at_key <= at_query + 128)
        visible = visible & (ed[0:1, 128 * block : 128 * block + 256] == query_docs)
        total = None
        for head, keys, vals in ((0, ka, va), (1, kb, vb)):
            scores = dot(q[rows, :], keys[:, span]) * 0.125
            scores = jnp.where(visible, scores, -jnp.inf)
            sink = sinks[head]
            top = jnp.maximum(jnp.max(scores, axis=1, keepdims=True), sink)
            raw = jnp.exp(scores - top)
            whole = jnp.sum(raw, axis=1, keepdims=True) + jnp.exp(sink - top)
            weights = (raw / whole).astype(BF16)
            part = dot_t(weights, vals[:, span])
            total = part if total is None else total + part
        att[rows, :] = total.astype(BF16)

    for block in (1, 2, 3):
        attend(block)
    gu_step(1)
    for copy in halo:
        copy.wait_recv()
    ka[0:64, 0:128] = hk[...]
    kb[64:128, 0:128] = hk[...]
    va[0:64, 0:128] = hv[...]
    vb[64:128, 0:128] = hv[...]
    ed[0:1, 0:128] = jnp.where(sp == 0, -1.0, dh[3:4, :].astype(F32))
    attend(0)
    lanes = pl.ds(pl.multiple_of(128 * tp, 128), 128)
    heads = []
    for j in range(1, 8):
        peer = lax.rem(tp + j, 8)
        rows = pl.ds(pl.multiple_of(64 * peer, 64), 64)
        heads.append(go(att.at[rows], at.at[:, lanes], (sp, peer)))
    own_rows = pl.ds(pl.multiple_of(64 * tp, 64), 64)
    at[:, lanes] = att[own_rows, :]
    gu_step(2)

    for copy in heads:
        copy.wait_recv()
    own_op.wait()
    for part in range(8):
        cols = pl.ds(256 * part, 256)
        mid[:, cols] = resid[:, cols].astype(F32) + dot(at[...], op[:, cols])
    rows64 = mid[...]
    scale = lax.rsqrt(jnp.mean(rows64 * rows64, axis=1, keepdims=True) + 1e-06)
    nb[own_rows, :] = (rows64 * scale * gain[...]).astype(BF16)
    rows_out = {}
    for j in (0, 1, 3, 2):
        where = partner if j == 0 else (sp, 2 * chip(j) + core)
        rows_out[j] = go(nb.at[own_rows], nb.at[own_rows], where)
    gu_step(3)
    gu_step(4)
    for half in (0, 1):
        for sign in BOTH:
            dn_first(half, sign, 1, dn.at[pl.ds(16 * half, 16)])
    for half in (0, 1):
        for sign in BOTH:
            for near in REL:
                far_gu[half, sign, near].wait_recv()
            for part in (0, 1):
                gu_send(2, half, sign, part)
    dn_step(1)

    def gu_pass(stage, part):
        for half in (0, 1):
            for sign in BOTH:
                far_gu[stage, half, sign, part].wait_recv()
                if stage < 3 or part == (0 if sign > 0 else 1):
                    gu_send(stage + 1, half, sign, part)

    passed = []

    def rows_on(j):
        rows_out[j].wait_recv()
        rows = pl.ds(pl.multiple_of(64 * (2 * chip(4 - j) + core), 64), 64)
        passed.append(go(nb.at[rows], nb.at[rows], partner))

    gu_pass(2, 0)
    rows_on(1)
    rows_on(3)
    gu_pass(2, 1)
    rows_on(2)
    dn_step(2)
    gu_pass(3, 0)
    gu_pass(3, 1)
    for copy in own_dn:
        copy.wait()
    for half in (0, 1):
        for sign in BOTH:
            dn_send(1, half, sign, 0)
    dn_step(3)
    dn_step(4)
    for half in (0, 1):
        for sign in BOTH:
            dn_send(1, half, sign, 1)
    rows_out[0].wait_recv()
    for copy in passed:
        copy.wait_recv()
    own_gu.wait()
    for half in (0, 1):
        for sign in BOTH:
            far_gu[4, half, sign, 0 if sign > 0 else 1].wait_recv()

    def columns(first, width):
        return wg[:, :, :, first : first + width].reshape(SIDE * SIDE * 32, width)

    def silu(v):
        return v / (1.0 + jnp.exp(-v))

    def hidden_part(i):
        gate = dot(nb[...], columns(256 * i, 256))
        if i < 2:
            up = dot(nb[...], columns(768 + 256 * i, 256))
            hid[:, 256 * i : 256 * (i + 1)] = (silu(gate) * up).astype(BF16)
            return
        up = dot(nb[...], columns(1280, 128))
        hid[:, 512:640] = (silu(gate[:, :128]) * up).astype(BF16)
        mixed = gate[:, 128:]
        lane = lax.broadcasted_iota(jnp.int32, mixed.shape, 1)
        ends = silu(mixed) * pltpu.roll(mixed, 64, 1)
        hid[:, 640:768] = jnp.where(lane < 64, ends, 0.0).astype(BF16)

    summed = {}

    def partial_of(stage):
        first = unit_of(stage, 0, 1)
        count = 2 if stage in (0, 4) else 4
        size, base = 64 * count, 128 * first
        units = wd[first : first + count].reshape(128 * count, 768)
        pb[base : base + 2 * size, :] = dot_t(units, hid[...]).astype(BF16)
        theirs = pl.ds(pl.multiple_of(base + size * other, 128), size)
        summed[stage] = go(pb.at[theirs], pr.at[pl.ds(64 * first, size)], partner)

    sums = []

    def chip_sum(stage):
        first = unit_of(stage, 0, 1)
        size = 128 if stage in (0, 4) else 256
        summed[stage].wait_recv()
        ours = pl.ds(pl.multiple_of(128 * first + size * core, 128), size)
        rows = pl.ds(64 * first, size)
        qb[rows, :] = (pb[ours, :].astype(F32) + pr[rows, :].astype(F32)).astype(BF16)
        for j in (2, 1, 3):
            tokens = pl.ds(pl.multiple_of(128 * chip(j), 128), 128)
            sums.append(go(qb.at[rows, tokens], rx.at[j - 1, rows], (sp, 2 * chip(j) + core)))

    hidden_part(0)
    hidden_part(1)
    dn_pass(1, 0)
    hidden_part(2)
    partial_of(0)
    dn_pass(1, 1)
    partial_of(1)
    chip_sum(0)
    chip_sum(1)
    dn_pass(2, 0)
    dn_pass(2, 1)
    partial_of(2)
    chip_sum(2)
    dn_pass(3, 0)
    dn_pass(3, 1)
    partial_of(3)
    chip_sum(3)
    for half in (0, 1):
        for sign in BOTH:
            far_dn[4, half, sign, 0 if sign > 0 else 1].wait_recv()
    partial_of(4)
    chip_sum(4)
    for copy in sums:
        copy.wait_recv()
    tokens = pl.ds(pl.multiple_of(128 * x, 128), 128)
    mine = qb[:, tokens].astype(F32)
    for j in range(3):
        mine = mine + rx[j].astype(F32)
    ss[core] = mine.astype(BF16)
    last = go(ss.at[core], ss.at[core], partner)
    last.wait_recv()
    fars = (0, -1, 1, -2, 2, -3, 3, -4)
    for half in (0, 1):
        for i, far in enumerate(fars):
            for r, near in enumerate(REL):
                dy, dz = (near, far) if half == 0 else (far, near)
                row = 256 * wrap(z, dz) + 32 * wrap(y, dy) + 16 * half
                first = 128 * i + 16 * r
                tn[pl.ds(pl.multiple_of(row, 16), 16), :] = ss[half, first : first + 16, :].astype(F32)
    for part in range(16):
        tt[:, 128 * part : 128 * (part + 1)] = tn[128 * part : 128 * (part + 1), :].T
    out[...] = (mid[...] + tt[pl.ds(pl.multiple_of(64 * core, 64), 64), :]).astype(BF16)
    for copy in pending:
        copy.wait_send()


def shards(
    resid, queries, keys, values, documents, sinks, out_proj, norm_gain, gate_proj, up_proj, down_proj
):
    gu = jnp.concatenate([gate_proj, up_proj[:, 640:], up_proj[:, :640]], axis=1)
    dn = jnp.pad(down_proj.T, ((0, 0), (0, 64)))
    vmem = pl.BlockSpec(memory_space=pltpu.VMEM)
    return pl.pallas_call(
        layer,
        out_shape=jax.ShapeDtypeStruct((64, 2048), BF16),
        in_specs=[pl.BlockSpec(memory_space=pltpu.SMEM)]
        + [vmem] * 8
        + [pl.BlockSpec(memory_space=pl.ANY)],
        out_specs=vmem,
        scratch_shapes=[
            pltpu.VMEM((8, 8, 32, 1408), BF16),
            pltpu.VMEM((16, 8, 16, 768), BF16),
            pltpu.VMEM((1024, 2048), BF16),
            pltpu.VMEM((512, 2048), BF16),
            pltpu.VMEM((64, 1024), BF16),
            pltpu.VMEM((128, 640), BF16),
            pltpu.VMEM((128, 640), BF16),
            pltpu.VMEM((128, 640), BF16),
            pltpu.VMEM((128, 640), BF16),
            pltpu.VMEM((64, 128), BF16),
            pltpu.VMEM((64, 128), BF16),
            pltpu.VMEM((4, 128), jnp.int32),
            pltpu.VMEM((8, 640), F32),
            pltpu.VMEM((512, 128), BF16),
            pltpu.VMEM((64, 2048), F32),
            pltpu.VMEM((512, 768), BF16),
            pltpu.VMEM((2048, 512), BF16),
            pltpu.VMEM((1024, 512), BF16),
            pltpu.VMEM((1024, 512), BF16),
            pltpu.VMEM((3, 1024, 128), BF16),
            pltpu.VMEM((2, 1024, 128), BF16),
            pltpu.VMEM((2048, 128), F32),
            pltpu.VMEM((128, 2048), F32),
            pltpu.SemaphoreType.DMA((SEMS,)),
            pltpu.SemaphoreType.DMA((SEMS,)),
            pltpu.SemaphoreType.DMA((4,)),
        ],
        compiler_params=pltpu.CompilerParams(
            collective_id=0, has_side_effects=True, vmem_limit_bytes=60 * 1024 * 1024
        ),
        name="layer",
    )(
        sinks, resid, queries, keys.T, values.T, documents.reshape(4, 128),
        norm_gain.reshape(1, 2048), gu, dn, out_proj,
    )


def solution(mesh):
    in_specs = (
        P(("sp", "tp"), None),
        P("sp", "tp"),
        P("sp", "tp"),
        P("sp", "tp"),
        P("sp"),
        P("tp"),
        P(),
        P(),
        P("sp", "tp"),
        P("sp", "tp"),
        P("tp", "sp"),
    )
    out_specs = P(("sp", "tp"), None)
    return jax.shard_map(shards, mesh=mesh, in_specs=in_specs, out_specs=out_specs, check_vma=False)
```

```python
import math

import jax
import jax.numpy as jnp
from jax import lax
from jax.experimental import pallas as pl
from jax.experimental.pallas import tpu as pltpu
from jax.sharding import PartitionSpec as P

MESH = pl.DeviceIdType.MESH
F32, BF16 = jnp.float32, jnp.bfloat16
SIDE = 8
REL = (0, -1, 1, -2, 2, -3, 3, -4)
LAST = {1: 4, -1: 3}
BOTH = (1, -1)
SEMS = 64
NEARS = ((0,), (-1, 1), (-2, 2), (-3, 3), (-4,))


def wrap(value, offset):
    return lax.rem(value + (offset + SIDE), SIDE) if offset else value


def unit_of(stage, half, sign):
    if stage == 0:
        return half
    if stage == 4:
        return 14 + half
    return 4 * stage - 2 + 2 * half + (0 if sign > 0 else 1)


def dot(a, b):
    return jnp.dot(a, b, preferred_element_type=F32)


def dot_t(a, b):
    return lax.dot_general(a, b, (((1,), (1,)), ((), ())), preferred_element_type=F32)


def layer(
    sinks, resid_hbm, q_hbm, kt_hbm, vt_hbm, docs_hbm, gain_hbm, gate_hbm, up_hbm, dt_hbm, op_hbm, out,
    resid, q, kt, vt, docs, gain, gate_own, up_own, dt_own, wg, wd, op, nb, at, ka, kb, va, vb, hk, hv, dh, ed, att, mid, hid,
    pb, pr, qb, rx, ss, tn, tt, send, recv, local,
):
    sp, tp = lax.axis_index("sp"), lax.axis_index("tp")
    y, z = lax.rem(sp, SIDE), lax.div(sp, SIDE)
    x, core = lax.rem(lax.div(tp, 2), 4), lax.rem(tp, 2)
    other = 1 - core
    partner = (sp, 2 * x + other)
    ahead = lax.rem(sp + 1, SIDE * SIDE)
    behind = lax.rem(sp + SIDE * SIDE - 1, SIDE * SIDE)

    def place(dy, dz):
        return (wrap(z, dz) * SIDE + wrap(y, dy), tp)

    def toward(half, ring, sign):
        return place(sign, 0) if half == ring else place(0, sign)

    def chip(j):
        return lax.rem(x + j, 4)

    barrier = pltpu.get_barrier_semaphore()
    greeted = [place(1, 0), place(-1, 0), place(0, 1), place(0, -1)]
    greeted += [(ahead, tp), (behind, tp)]
    greeted += [(sp, lax.rem(tp + j, 8)) for j in range(1, 8)]
    for where in greeted:
        pl.semaphore_signal(barrier, inc=1, device_id=where, device_id_type=MESH)

    loads = [
        pltpu.make_async_copy(src, dst, local.at[i])
        for i, (src, dst) in enumerate(
            (
                (gate_hbm, gate_own), (up_hbm, up_own), (dt_hbm, dt_own), (kt_hbm, kt), (vt_hbm, vt),
                (docs_hbm, docs), (q_hbm, q), (resid_hbm, resid), (gain_hbm, gain), (op_hbm, op),
            )
        )
    ]
    for copy in loads:
        copy.start()
    for copy in loads[:3]:
        copy.wait()
    wg[z, y, :, 0:640] = gate_own[:, 0:640]
    wg[z, y, :, 768:1408] = up_own[:, 0:640]
    wg[z, y, :, 640:768] = jnp.concatenate([gate_own[:, 640:704], up_own[:, 640:704]], axis=1)
    for half in (0, 1):
        rows = slice(16 * half, 16 * half + 16)
        wd[half, 0, :, 0:640] = dt_own[rows, 0:640]
        ends = [dt_own[rows, 640:704], jnp.zeros((16, 64), BF16)]
        wd[half, 0, :, 640:768] = jnp.concatenate(ends, axis=1)
    for copy in loads[3:7]:
        copy.wait()
    pl.semaphore_wait(barrier, len(greeted))

    arrivals, leaves = {}, {}

    def index_in(table, name, amount):
        entry = table.setdefault(name, [len(table), 0])
        entry[1] += amount
        return entry[0]

    def go(name, leave, src, dst, where):
        amount = math.prod(src.shape)
        pltpu.make_async_remote_copy(
            src_ref=src, dst_ref=dst,
            send_sem=send.at[index_in(leaves, leave, amount)],
            recv_sem=recv.at[index_in(arrivals, name, amount)],
            device_id=where, device_id_type=MESH,
        ).start()

    def whole(table, name, like):
        place_of, amount = table[name]
        assert amount == math.prod(like.shape), (name, amount, like.shape)
        return pltpu.make_async_remote_copy(
            src_ref=like, dst_ref=like, send_sem=send.at[place_of], recv_sem=recv.at[place_of],
            device_id=partner, device_id_type=MESH,
        )

    def arrived(name, like):
        whole(arrivals, name, like).wait_recv()

    def left(name, like):
        whole(leaves, name, like).wait_send()

    def gu_far(half, near, far):
        dy, dz = (near, far) if half == 0 else (far, near)
        return wg.at[wrap(z, dz), wrap(y, dy), pl.ds(16 * half, 16)]

    def group_of(near):
        return next(group for group in NEARS if near in group)

    def gu_send(stage, half, sign, near):
        block = gu_far(half, near, -sign * (stage - 1))
        name = ("gu", stage, group_of(near) if stage < 4 else None)
        go(name, ("gu", stage), block, block, toward(half, 1, sign))

    def gu_first(half, sign, k):
        block = gu_far(half, -sign * (k - 1), 0)
        go(("gu first", k), "gu first", block, block, toward(half, 0, sign))

    def gu_step(k):
        arrived(("gu first", k), wg.at[0, 0 : 2 if k < 4 else 1])
        for half in (0, 1):
            for sign in BOTH:
                if k < LAST[sign]:
                    gu_first(half, sign, k + 1)
        for half in (0, 1):
            for sign in BOTH:
                if k <= LAST[sign]:
                    for way in BOTH:
                        gu_send(1, half, way, -sign * k)

    def gu_pass(stage, *nears):
        arrived(("gu", stage, nears), wg.at[0, 0 : 2 * len(nears)])
        for near in nears:
            for half in (0, 1):
                for sign in BOTH:
                    if stage < 3 or (near >= 0) == (sign > 0):
                        gu_send(stage + 1, half, sign, near)

    def dn_first(half, sign, k):
        src = wd.at[half, REL.index(-sign * (k - 1))]
        dst = wd.at[half, REL.index(-sign * k)]
        go(("dn first", k), "dn first", src, dst, toward(half, 0, sign))

    def dn_step(k):
        arrived(("dn first", k), wd.at[0, 0 : 4 if k < 4 else 2])
        for half in (0, 1):
            for sign in BOTH:
                if k < LAST[sign]:
                    dn_first(half, sign, k + 1)

    def dn_send(stage, half, sign, part):
        some = pl.ds(4 * part, 4)
        if stage == 4:
            some = pl.ds(4 * part + (0 if sign > 0 else 2), 2)
        src = wd.at[unit_of(stage - 1, half, sign), some]
        dst = wd.at[unit_of(stage, half, sign), some]
        go(("dn", stage, part), "dn", src, dst, toward(half, 1, sign))

    def dn_start(part):
        for half in (0, 1):
            for sign in BOTH:
                dn_send(1, half, sign, part)

    def dn_pass(stage, part):
        arrived(("dn", stage, part), wd.at[0:2] if stage < 4 else wd.at[0])
        if stage < 4:
            for half in (0, 1):
                for sign in BOTH:
                    dn_send(stage + 1, half, sign, part)

    for half in (0, 1):
        for sign in BOTH:
            gu_first(half, sign, 1)
    for half in (0, 1):
        for sign in BOTH:
            dn_first(half, sign, 1)
    for half in (0, 1):
        for sign in BOTH:
            gu_send(1, half, sign, 0)
    tail = pl.ds(384, 128)
    go("halo", "halo", kt.at[:, tail], hk, (ahead, tp))
    go("halo", "halo", vt.at[:, tail], hv, (ahead, tp))
    go("docs", "docs", docs, dh, (ahead, tp))

    for first, second, source in ((ka, kb, kt), (va, vb, vt)):
        first[64:128, :] = jnp.zeros((64, 640), BF16)
        second[0:64, :] = jnp.zeros((64, 640), BF16)
        first[0:64, 128:640] = source[...]
        second[64:128, 128:640] = source[...]
    for block in range(4):
        ed[0:1, 128 * (block + 1) : 128 * (block + 2)] = docs[block : block + 1, :].astype(F32)

    def attend(block):
        rows, span = pl.ds(128 * block, 128), pl.ds(128 * block, 256)
        query_docs = jnp.broadcast_to(ed[0:1, 128 * (block + 1) : 128 * (block + 2)], (128, 128)).T
        query_docs = jnp.concatenate([query_docs, query_docs], axis=1)
        at_query = lax.broadcasted_iota(jnp.int32, (128, 256), 0)
        at_key = lax.broadcasted_iota(jnp.int32, (128, 256), 1)
        visible = (at_key > at_query) & (at_key <= at_query + 128)
        visible = visible & (ed[0:1, 128 * block : 128 * block + 256] == query_docs)
        total = None
        for head, keys, vals in ((0, ka, va), (1, kb, vb)):
            scores = dot(q[rows, :], keys[:, span]) * 0.125
            scores = jnp.where(visible, scores, -jnp.inf)
            sink = sinks[head]
            top = jnp.maximum(jnp.max(scores, axis=1, keepdims=True), sink)
            raw = jnp.exp(scores - top)
            whole = jnp.sum(raw, axis=1, keepdims=True) + jnp.exp(sink - top)
            weights = (raw / whole).astype(BF16)
            part = dot_t(weights, vals[:, span])
            total = part if total is None else total + part
        att[rows, :] = total.astype(BF16)

    for block in (1, 2, 3):
        attend(block)
    gu_step(1)
    dn_step(1)
    gu_pass(1, 0)
    gu_step(2)
    gu_pass(1, -1, 1)
    dn_step(2)
    gu_pass(2, 0)
    arrived("halo", kt.at[:, 0:256])
    arrived("docs", dh)
    ka[0:64, 0:128] = hk[...]
    kb[64:128, 0:128] = hk[...]
    va[0:64, 0:128] = hv[...]
    vb[64:128, 0:128] = hv[...]
    ed[0:1, 0:128] = jnp.where(sp == 0, -1.0, dh[3:4, :].astype(F32))
    attend(0)
    lanes = pl.ds(pl.multiple_of(128 * tp, 128), 128)
    for j in range(1, 8):
        peer = lax.rem(tp + j, 8)
        rows = pl.ds(pl.multiple_of(64 * peer, 64), 64)
        go("heads", "heads", att.at[rows], at.at[:, lanes], (sp, peer))
    own_rows = pl.ds(pl.multiple_of(64 * tp, 64), 64)
    at[:, lanes] = att[own_rows, :]
    gu_step(3)
    gu_pass(1, -2, 2)
    gu_pass(2, -1, 1)
    dn_step(3)
    gu_pass(3, 0)

    arrived("heads", att.at[0:448])
    for copy in loads[7:]:
        copy.wait()
    for part in range(8):
        cols = pl.ds(256 * part, 256)
        mid[:, cols] = resid[:, cols].astype(F32) + dot(at[...], op[:, cols])
    rows64 = mid[...]
    scale = lax.rsqrt(jnp.mean(rows64 * rows64, axis=1, keepdims=True) + 1e-06)
    nb[own_rows, :] = (rows64 * scale * gain[...]).astype(BF16)
    for j in (0, 1, 3, 2):
        where = partner if j == 0 else (sp, 2 * chip(j) + core)
        go(("rows", j), "rows", nb.at[own_rows], nb.at[own_rows], where)

    def rows_on(j):
        arrived(("rows", j), nb.at[0:64])
        rows = pl.ds(pl.multiple_of(64 * (2 * chip(4 - j) + core), 64), 64)
        go(("rows", 0), "rows", nb.at[rows], nb.at[rows], partner)

    gu_step(4)
    gu_pass(1, -3, 3)
    gu_pass(2, -2, 2)
    gu_pass(3, -1, 1)
    dn_step(4)
    gu_pass(1, -4)
    gu_pass(2, -3, 3)
    gu_pass(3, -2, 2)
    rows_on(1)
    rows_on(3)
    gu_pass(2, -4)
    dn_start(0)
    gu_pass(3, -3, 3)
    rows_on(2)
    gu_pass(3, -4)
    dn_start(1)
    dn_pass(1, 0)
    arrived(("rows", 0), nb.at[0:256])
    arrived(("gu", 4, None), wg.at[0])

    def columns(first, width):
        return wg[:, :, :, first : first + width].reshape(SIDE * SIDE * 32, width)

    def silu(v):
        return v / (1.0 + jnp.exp(-v))

    def hidden_part(i):
        gate = dot(nb[...], columns(256 * i, 256))
        if i < 2:
            up = dot(nb[...], columns(768 + 256 * i, 256))
            hid[:, 256 * i : 256 * (i + 1)] = (silu(gate) * up).astype(BF16)
            return
        up = dot(nb[...], columns(1280, 128))
        hid[:, 512:640] = (silu(gate[:, :128]) * up).astype(BF16)
        mixed = gate[:, 128:]
        lane = lax.broadcasted_iota(jnp.int32, mixed.shape, 1)
        ends = silu(mixed) * pltpu.roll(mixed, 64, 1)
        hid[:, 640:768] = jnp.where(lane < 64, ends, 0.0).astype(BF16)

    def partial_of(stage):
        first = unit_of(stage, 0, 1)
        count = 2 if stage in (0, 4) else 4
        size, base = 64 * count, 128 * first
        units = wd[first : first + count].reshape(128 * count, 768)
        pb[base : base + 2 * size, :] = dot_t(units, hid[...]).astype(BF16)
        theirs = pl.ds(pl.multiple_of(base + size * other, 128), size)
        go(("pair", stage), "pair", pb.at[theirs], pr.at[pl.ds(64 * first, size)], partner)

    def chip_sum(stage):
        first = unit_of(stage, 0, 1)
        size = 128 if stage in (0, 4) else 256
        arrived(("pair", stage), pr.at[0:size])
        ours = pl.ds(pl.multiple_of(128 * first + size * core, 128), size)
        rows = pl.ds(64 * first, size)
        qb[rows, :] = (pb[ours, :].astype(F32) + pr[rows, :].astype(F32)).astype(BF16)
        for j in (2, 1, 3):
            tokens = pl.ds(pl.multiple_of(128 * chip(j), 128), 128)
            where = (sp, 2 * chip(j) + core)
            go(("sums", stage == 4), "sums", qb.at[rows, tokens], rx.at[j - 1, rows], where)

    tokens = pl.ds(pl.multiple_of(128 * x, 128), 128)

    def finish(ending):
        rows = slice(896, 1024) if ending else slice(0, 896)
        arrived(("sums", ending), rx.at[:, rows])
        mine = qb[rows, tokens].astype(F32)
        for j in range(3):
            mine = mine + rx[j, rows].astype(F32)
        ss[core, rows] = mine.astype(BF16)
        done = ss.at[core, rows]
        go(("last", ending), "last", done, done, partner)

    hidden_part(0)
    hidden_part(1)
    dn_pass(1, 1)
    hidden_part(2)
    partial_of(0)
    dn_pass(2, 0)
    partial_of(1)
    chip_sum(0)
    dn_pass(2, 1)
    chip_sum(1)
    partial_of(2)
    dn_pass(3, 0)
    chip_sum(2)
    dn_pass(3, 1)
    partial_of(3)
    chip_sum(3)
    dn_pass(4, 0)
    dn_pass(4, 1)
    partial_of(4)
    chip_sum(4)
    finish(False)
    finish(True)
    arrived(("last", False), ss.at[0, 0:896])
    arrived(("last", True), ss.at[0, 0:128])
    fars = (0, -1, 1, -2, 2, -3, 3, -4)
    for half in (0, 1):
        for i, far in enumerate(fars):
            for r, near in enumerate(REL):
                dy, dz = (near, far) if half == 0 else (far, near)
                row = 256 * wrap(z, dz) + 32 * wrap(y, dy) + 16 * half
                first = 128 * i + 16 * r
                tn[pl.ds(pl.multiple_of(row, 16), 16), :] = ss[half, first : first + 16, :].astype(F32)
    for part in range(16):
        tt[:, 128 * part : 128 * (part + 1)] = tn[128 * part : 128 * (part + 1), :].T
    out[...] = (mid[...] + tt[pl.ds(pl.multiple_of(64 * core, 64), 64), :]).astype(BF16)
    left("gu first", wg.at[0, 0:7])
    for stage in (1, 2, 3):
        left(("gu", stage), wg.at[0:2])
    left(("gu", 4), wg.at[0])
    left("dn first", wd.at[0:2, 0:7])
    left("dn", wd.at[0:14])
    left("halo", kt.at[:, 0:256])
    left("docs", dh)
    left("heads", att.at[0:448])
    left("rows", nb.at[0:448])
    left("pair", pr)
    left("sums", rx)
    left("last", ss.at[0])
    assert max(len(arrivals), len(leaves)) <= SEMS, (len(arrivals), len(leaves))


def shards(
    resid, queries, keys, values, documents, sinks, out_proj, norm_gain, gate_proj, up_proj, down_proj
):
    vmem = pl.BlockSpec(memory_space=pltpu.VMEM)
    return pl.pallas_call(
        layer,
        out_shape=jax.ShapeDtypeStruct((64, 2048), BF16),
        in_specs=[pl.BlockSpec(memory_space=pltpu.SMEM)]
        + [pl.BlockSpec(memory_space=pl.ANY)] * 10,
        out_specs=vmem,
        scratch_shapes=[
            pltpu.VMEM((64, 2048), BF16),
            pltpu.VMEM((512, 128), BF16),
            pltpu.VMEM((64, 512), BF16),
            pltpu.VMEM((64, 512), BF16),
            pltpu.VMEM((4, 128), jnp.int32),
            pltpu.VMEM((1, 2048), F32),
            pltpu.VMEM((32, 704), BF16),
            pltpu.VMEM((32, 704), BF16),
            pltpu.VMEM((32, 704), BF16),
            pltpu.VMEM((8, 8, 32, 1408), BF16),
            pltpu.VMEM((16, 8, 16, 768), BF16),
            pltpu.VMEM((1024, 2048), BF16),
            pltpu.VMEM((512, 2048), BF16),
            pltpu.VMEM((64, 1024), BF16),
            pltpu.VMEM((128, 640), BF16),
            pltpu.VMEM((128, 640), BF16),
            pltpu.VMEM((128, 640), BF16),
            pltpu.VMEM((128, 640), BF16),
            pltpu.VMEM((64, 128), BF16),
            pltpu.VMEM((64, 128), BF16),
            pltpu.VMEM((4, 128), jnp.int32),
            pltpu.VMEM((8, 640), F32),
            pltpu.VMEM((512, 128), BF16),
            pltpu.VMEM((64, 2048), F32),
            pltpu.VMEM((512, 768), BF16),
            pltpu.VMEM((2048, 512), BF16),
            pltpu.VMEM((1024, 512), BF16),
            pltpu.VMEM((1024, 512), BF16),
            pltpu.VMEM((3, 1024, 128), BF16),
            pltpu.VMEM((2, 1024, 128), BF16),
            pltpu.VMEM((2048, 128), F32),
            pltpu.VMEM((128, 2048), F32),
            pltpu.SemaphoreType.DMA((SEMS,)),
            pltpu.SemaphoreType.DMA((SEMS,)),
            pltpu.SemaphoreType.DMA((10,)),
        ],
        compiler_params=pltpu.CompilerParams(
            collective_id=0, has_side_effects=True, vmem_limit_bytes=60 * 1024 * 1024
        ),
        name="layer",
    )(
        sinks, resid, queries, keys.T, values.T, documents.reshape(4, 128),
        norm_gain.reshape(1, 2048), gate_proj, up_proj, down_proj.T, out_proj,
    )


def solution(mesh):
    in_specs = (
        P(("sp", "tp"), None),
        P("sp", "tp"),
        P("sp", "tp"),
        P("sp", "tp"),
        P("sp"),
        P("tp"),
        P(),
        P(),
        P("sp", "tp"),
        P("sp", "tp"),
        P("tp", "sp"),
    )
    out_specs = P(("sp", "tp"), None)
    return jax.shard_map(shards, mesh=mesh, in_specs=in_specs, out_specs=out_specs, check_vma=False)
```
